32 devices in a mesh: rep: 2 (over x), fs: 4 (over z), tp: 4 (over y, core).
Axes of the slice: x: 2, y: 2, z: 4, core: 2. Of those that a mesh axis runs over, the one named last changes fastest.
Arguments:
- residual: bfloat16 [8, 768, 4, 512], P(('rep', 'fs'), None, None, 'tp'), may hold values from -6 to 6
- mixer_gain: float32 [4, 512], P(None, 'tp'), may hold values from 0.1 to 1.9
- pool_weight: float32 [4, 512, 512], P(None, 'fs', 'tp'), may hold values from -0.25 to 0.25
- pool_scale: float32 [4, 512], P(None, 'tp'), may hold values from 0.5 to 2
- channel_gain: float32 [4, 512], P(None, 'tp'), may hold values from 0.1 to 1.9
- gate_weight: float32 [2048, 6144], P('fs', 'tp'), may hold values from -0.125 to 0.125
- up_weight: float32 [2048, 6144], P('fs', 'tp'), may hold values from -0.125 to 0.125
- gate_scale: float32 [4, 1536], P('fs', 'tp'), may hold values from 0.5 to 2
- up_scale: float32 [4, 1536], P('fs', 'tp'), may hold values from 0.5 to 2
- gate_taps: float32 [3, 6144], P(None, 'tp'), may hold values from -3.5 to 3.5
- up_taps: float32 [3, 6144], P(None, 'tp'), may hold values from -3.5 to 3.5
- down_weight: float32 [6144, 2048], P('tp', 'fs'), may hold values from -0.078125 to 0.078125
- down_scale: float32 [4, 512], P(None, 'tp'), may hold values from 0.5 to 2
Outputs:
- layer_out: bfloat16 [8, 768, 4, 512], P(('rep', 'fs'), None, None, 'tp')
The draws below stay inside these ranges and needn't reach their ends.
All inputs are finite; a program needn't handle non-finite values.
Results may differ from the reference program's by a relative error of at most 0.018.
Values may be sent and summed in bfloat16 or wider, within the bound.
A program may use at most 128 MiB of HBM per device.

```python
import math
import jax
import jax.numpy as jnp
from jax import lax

D = 2048
G = 4
C = 512
FF = 6144
SEQ_LEN = 768
SEQS = 8
N_FS = 4
N_TP = 4


def level_of(own_key, shape, shards, least, largest):
    level = 1.0
    for position, parts in shards:
        draws = jax.random.uniform(jax.random.fold_in(jax.random.fold_in(own_key, 6), position), (parts,), jnp.float32, least / len(shards), largest / len(shards))
        level = level * jnp.repeat(jnp.exp(draws), shape[position] // parts).reshape((-1,) + (1,) * (len(shape) - 1 - position))
    return level


def gaussian(rng, shape, scale, reach, shards=(), kind=jnp.bfloat16):
    level = level_of(rng, shape, shards, -0.22, 0.18) if shards else 1.0
    values = jax.random.normal(rng, shape, jnp.float32) * scale * level
    return jnp.minimum(jnp.maximum(values, -reach), reach).astype(kind)


def setup_inputs(seed: int = 0) -> dict:
    key_list = jax.random.split(jax.random.key(seed), 14)
    residual = gaussian(key_list[0], (SEQS, SEQ_LEN, G, C), 1.0, 6.0, ((0, 8), (3, 4)))
    mixer_gain = jnp.clip(1.0 + 0.18 * jax.random.normal(key_list[1], (G, C), jnp.float32), 0.1, 1.9)
    pool_weight = gaussian(key_list[2], (G, C, C), C ** -0.5, 0.25, ((1, 4), (2, 4)), jnp.float32)
    pool_scale = jnp.clip(jnp.exp(math.log(2.0) - 1.3862944 * jax.random.uniform(key_list[3], (G, C), jnp.float32) ** level_of(key_list[3], (G, C), ((1, 4),), -0.2, 0.2)), 0.5, 2.0)
    channel_gain = jnp.clip(1.0 + 0.18 * jax.random.normal(key_list[4], (G, C), jnp.float32), 0.1, 1.9)
    gate_weight = gaussian(key_list[5], (D, FF), D ** -0.5, 0.125, ((0, 4), (1, 4)), jnp.float32)
    up_weight = gaussian(key_list[6], (D, FF), D ** -0.5, 0.125, ((0, 4), (1, 4)), jnp.float32)
    gate_scale = jnp.clip(jnp.exp(math.log(2.0) - 1.3862944 * jax.random.uniform(key_list[7], (N_FS, FF // N_FS), jnp.float32) ** level_of(key_list[7], (N_FS, FF // N_FS), ((0, 4), (1, 4)), -0.2, 0.2)), 0.5, 2.0)
    up_scale = jnp.clip(jnp.exp(math.log(2.0) - 1.3862944 * jax.random.uniform(key_list[8], (N_FS, FF // N_FS), jnp.float32) ** level_of(key_list[8], (N_FS, FF // N_FS), ((0, 4), (1, 4)), -0.2, 0.2)), 0.5, 2.0)
    gate_taps = gaussian(key_list[9], (3, FF), 3 ** -0.5, 3.5, ((1, 4),), jnp.float32)
    up_taps = gaussian(key_list[10], (3, FF), 3 ** -0.5, 3.5, ((1, 4),), jnp.float32)
    down_weight = gaussian(key_list[11], (FF, D), FF ** -0.5, 0.078125, ((0, 4), (1, 4)), jnp.float32)
    down_scale = jnp.clip(jnp.exp(math.log(2.0) - 1.3862944 * jax.random.uniform(key_list[12], (G, C), jnp.float32) ** level_of(key_list[12], (G, C), ((1, 4),), -0.2, 0.2)), 0.5, 2.0)
    return dict(residual=residual, mixer_gain=mixer_gain, pool_weight=pool_weight, pool_scale=pool_scale, channel_gain=channel_gain, gate_weight=gate_weight, up_weight=up_weight, gate_scale=gate_scale, up_scale=up_scale, gate_taps=gate_taps, up_taps=up_taps, down_weight=down_weight, down_scale=down_scale)


WINDOWS = (2, 4, 8, 16)
EPSILON = 1e-05

def shifted(values, steps):
    padding = jnp.zeros((steps,) + values.shape[1:], values.dtype)
    return jnp.concatenate([padding, values[:-steps]], axis=0)

def pooled_groups(normed):
    values = normed.astype(jnp.float32)
    totals = values
    reach_now = 1
    columns = []
    positions = jnp.arange(1, values.shape[0] + 1).astype(jnp.float32)
    for group_idx in range(len(WINDOWS)):
        while reach_now < WINDOWS[group_idx]:
            totals = totals + shifted(totals, reach_now)
            reach_now = reach_now * 2
        divisor = jnp.minimum(positions, float(WINDOWS[group_idx]))
        columns.append(totals[:, group_idx] / divisor[:, None] - values[:, group_idx])
    return jnp.stack(columns, axis=1).astype(jnp.bfloat16)

def normalized(residual, gain):
    values = residual.astype(jnp.float32)
    mean_square = lax.optimization_barrier(jnp.mean(values * values, axis=(1, 2), keepdims=True))
    return (values * lax.rsqrt(mean_square + EPSILON) * gain).astype(jnp.bfloat16)

def causal_taps(stored, taps):
    values = stored.astype(jnp.float32)
    return taps[2] * values + taps[1] * shifted(values, 1) + taps[0] * shifted(values, 2)

def shard_order(scale):
    return jnp.transpose(scale.reshape(N_FS, N_TP, -1), (1, 0, 2)).reshape(-1)

def one_sequence(residual, mixer_gain, pool_half, pool_scale, channel_gain, gate_half, up_half, gate_columns, up_columns, gate_taps, up_taps, down_half, down_scale):
    normed = normalized(residual, mixer_gain)
    pooled = pooled_groups(normed)
    mixed = jnp.einsum('lgc,gce->lge', pooled.astype(jnp.float32), pool_half.astype(jnp.float32))
    middle = (mixed * pool_scale + residual.astype(jnp.float32)).astype(jnp.bfloat16)
    length = middle.shape[0]
    inputs = normalized(middle, channel_gain).reshape(length, -1)
    gate_pre = (jnp.dot(inputs, gate_half, preferred_element_type=jnp.float32) * gate_columns).astype(jnp.bfloat16)
    up_pre = (jnp.dot(inputs, up_half, preferred_element_type=jnp.float32) * up_columns).astype(jnp.bfloat16)
    hidden = (jax.nn.silu(causal_taps(gate_pre, gate_taps)) * causal_taps(up_pre, up_taps)).astype(jnp.bfloat16)
    block_rows = hidden.shape[1] // N_TP
    summed = jnp.zeros((length, down_half.shape[1]), jnp.float32)
    for shard_idx in range(N_TP):
        lower = shard_idx * block_rows
        partial_sum = jnp.dot(hidden[:, lower:lower + block_rows], down_half[lower:lower + block_rows], preferred_element_type=jnp.float32).astype(jnp.bfloat16)
        summed = summed + lax.optimization_barrier(partial_sum).astype(jnp.float32)
    summed = summed.reshape(middle.shape)
    return (summed * down_scale + middle.astype(jnp.float32)).astype(jnp.bfloat16)

def reference(residual, mixer_gain, pool_weight, pool_scale, channel_gain, gate_weight, up_weight, gate_scale, up_scale, gate_taps, up_taps, down_weight, down_scale):
    pool_half = pool_weight.astype(jnp.bfloat16)
    gate_half = gate_weight.astype(jnp.bfloat16)
    up_half = up_weight.astype(jnp.bfloat16)
    down_half = down_weight.astype(jnp.bfloat16)
    gate_columns = shard_order(gate_scale)
    up_columns = shard_order(up_scale)

    def per_sequence(sequence):
        return one_sequence(sequence, mixer_gain, pool_half, pool_scale, channel_gain, gate_half, up_half, gate_columns, up_columns, gate_taps, up_taps, down_half, down_scale)
    return lax.map(per_sequence, residual)
```

```python
import functools

import jax
import jax.numpy as jnp
from jax import lax
from jax.experimental import pallas as pl
from jax.experimental.pallas import tpu as pltpu
from jax.sharding import PartitionSpec as P

WINDOWS = (2, 4, 8, 16)
EPSILON = 1e-05
SUBS = 2
COLUMNS = 256
F32 = jnp.float32
BF16 = jnp.bfloat16


def delayed(values, steps):
    rows = lax.broadcasted_iota(jnp.int32, values.shape, 0)
    return jnp.where(rows >= steps, pltpu.roll(values, steps, 0), 0.0)


def causal_taps(values, taps):
    return taps[2:3] * values + taps[1:2] * delayed(values, 1) + taps[0:1] * delayed(values, 2)


def block_kernel(
    sizes,
    residual,
    gains,
    pool_scale,
    down_scale,
    scale_pair,
    gate_taps,
    up_taps,
    pool_own,
    gate_own,
    up_own,
    down_own,
    out,
    pool_full,
    gate_full,
    up_full,
    down_full,
    gathered,
    middle_all,
    gains_all,
    scales_all,
    scale_row,
    pooled,
    middle,
    inputs,
    gate_pre,
    hidden,
    partials,
    arrived,
    ring_send,
    ring_recv,
    rep_send,
    rep_recv,
    pool_send,
    pool_recv,
    pool_rep_send,
    pool_rep_recv,
    scale_send,
    scale_recv,
    tp_send,
    tp_recv,
    part_send,
    part_recv,
    local_sem,
):
    n_rep, n_fs, n_tp = sizes
    rep, fs, tp = (lax.axis_index(name) for name in ("rep", "fs", "tp"))
    length = residual.shape[0]
    groups = pool_full.shape[0]
    channels = pool_full.shape[1]
    local = residual.shape[1] // groups
    width = groups * channels

    def other(axis, offset):
        me, count = {"rep": (rep, n_rep), "fs": (fs, n_fs), "tp": (tp, n_tp)}[axis]
        return lax.rem(me + offset, count)

    def remote(src, dst, send, recv, axis, offset):
        return pltpu.make_async_remote_copy(
            src_ref=src,
            dst_ref=dst,
            send_sem=send,
            recv_sem=recv,
            device_id={axis: other(axis, offset)},
            device_id_type=pl.DeviceIdType.MESH,
        )

    barrier = pltpu.get_barrier_semaphore()
    for axis, count in (("rep", n_rep), ("fs", n_fs), ("tp", n_tp)):
        for offset in range(1, count):
            pl.semaphore_signal(
                barrier,
                inc=1,
                device_id={axis: other(axis, offset)},
                device_id_type=pl.DeviceIdType.MESH,
            )
    pl.semaphore_wait(barrier, n_rep + n_fs + n_tp - 3)

    sent = []

    def start(copy):
        copy.start()
        sent.append(copy)

    weights = ((gate_own, gate_full), (up_own, up_full), (down_own, down_full))

    def piece(w, shard, half, sub, own=False):
        rows = weights[w][0].shape[0] // (n_rep * SUBS)
        part = pl.ds(pl.multiple_of((half * SUBS + sub) * rows, rows), rows)
        return weights[w][0].at[part] if own else weights[w][1].at[shard, part]

    def ring(w, sub, step):
        shard = lax.rem(fs - step + n_fs, n_fs)
        return remote(
            piece(w, shard, rep, sub, own=step == 0),
            piece(w, shard, rep, sub),
            ring_send.at[w, sub, step],
            ring_recv.at[w, sub, step],
            "fs",
            1,
        )

    def serve(w, sub, step):
        shard = lax.rem(fs - step - 1 + n_fs, n_fs)
        mine = piece(w, shard, rep, sub)
        remote(
            mine, mine, ring_send.at[w, sub, step], ring_recv.at[w, sub, step], "fs", 1
        ).wait_recv()
        for d in range(1, n_rep):
            start(
                remote(
                    mine,
                    mine,
                    rep_send.at[w, sub, step, d - 1],
                    rep_recv.at[w, sub, step, d - 1],
                    "rep",
                    d,
                )
            )
        if step < n_fs - 2:
            start(ring(w, sub, step + 1))

    def settle(w, step):
        shard = lax.rem(fs - step - 1 + n_fs, n_fs)
        for sub in range(SUBS):
            for d in range(1, n_rep):
                got = piece(w, shard, other("rep", n_rep - d), sub)
                remote(
                    got,
                    got,
                    rep_send.at[w, sub, step, d - 1],
                    rep_recv.at[w, sub, step, d - 1],
                    "rep",
                    d,
                ).wait_recv()

    def local_copy(src, dst, idx):
        copy = pltpu.make_async_copy(src, dst, local_sem.at[idx])
        copy.start()
        return copy

    own_copies = [
        local_copy(residual, gathered.at[tp], 0),
        local_copy(gains, gains_all.at[tp], 1),
        local_copy(scale_pair, scales_all.at[fs], 2),
        local_copy(gate_own, gate_full.at[fs], 3),
        local_copy(up_own, up_full.at[fs], 4),
        local_copy(down_own, down_full.at[fs], 5),
    ]

    pool_rows = pool_own.shape[1]
    rep_groups = groups // n_rep

    def pool_part(shard, half):
        return pool_full.at[
            pl.ds(half * rep_groups, rep_groups),
            pl.ds(pl.multiple_of(shard * pool_rows, pool_rows), pool_rows),
        ]

    pool_copy = local_copy(
        pool_own, pool_full.at[:, pl.ds(pl.multiple_of(fs * pool_rows, pool_rows), pool_rows)], 6
    )

    for d in range(1, n_fs):
        start(
            remote(
                pool_own.at[pl.ds(rep * rep_groups, rep_groups)],
                pool_part(fs, rep),
                pool_send.at[d - 1],
                pool_recv.at[d - 1],
                "fs",
                d,
            )
        )
    for w in (0, 1):
        for sub in range(SUBS):
            if n_fs > 1:
                start(ring(w, sub, 0))
    for d in range(1, n_tp):
        start(remote(gains, gains_all.at[tp], tp_send.at[0, d - 1], tp_recv.at[0, d - 1], "tp", d))
    for d in range(1, n_tp):
        start(
            remote(residual, gathered.at[tp], tp_send.at[1, d - 1], tp_recv.at[1, d - 1], "tp", d)
        )
    for d in range(1, n_fs):
        start(
            remote(
                scale_pair, scales_all.at[fs], scale_send.at[d - 1], scale_recv.at[d - 1], "fs", d
            )
        )

    for d in range(1, n_fs):
        shard = other("fs", n_fs - d)
        mine = pool_part(shard, rep)
        remote(mine, mine, pool_send.at[d - 1], pool_recv.at[d - 1], "fs", d).wait_recv()
        for e in range(1, n_rep):
            start(
                remote(
                    mine,
                    mine,
                    pool_rep_send.at[d - 1, e - 1],
                    pool_rep_recv.at[d - 1, e - 1],
                    "rep",
                    e,
                )
            )
    for d in range(1, n_fs):
        shard = other("fs", n_fs - d)
        for e in range(1, n_rep):
            got = pool_part(shard, other("rep", n_rep - e))
            remote(
                got,
                got,
                pool_rep_send.at[d - 1, e - 1],
                pool_rep_recv.at[d - 1, e - 1],
                "rep",
                e,
            ).wait_recv()
    pool_copy.wait()
    for copy in own_copies:
        copy.wait()

    def tp_arrivals(idx, buffer):
        for d in range(1, n_tp):
            got = buffer.at[other("tp", n_tp - d)]
            remote(got, got, tp_send.at[idx, d - 1], tp_recv.at[idx, d - 1], "tp", d).wait_recv()

    for sub in range(SUBS):
        serve(0, sub, 0)
    tp_arrivals(0, gains_all)
    tp_arrivals(1, gathered)
    for sub in range(SUBS):
        serve(1, sub, 0)

    def mean_square_root(buffer):
        total = jnp.zeros((length, 1), F32)
        for t in range(n_tp):
            values = buffer[t].astype(F32)
            total = total + jnp.sum(values * values, axis=1, keepdims=True)
        return lax.rsqrt(total / width + EPSILON)

    factor = mean_square_root(gathered)
    positions = lax.broadcasted_iota(jnp.int32, (length, 1), 0).astype(F32) + 1.0
    for g in range(groups):
        part = slice(g * local, (g + 1) * local)
        share = 1.0 / jnp.minimum(positions, float(WINDOWS[g]))
        for t in range(n_tp):
            values = gathered[t, :, part].astype(F32)
            normed = (values * factor * gains_all[t, 0:1, part]).astype(BF16).astype(F32)
            totals = normed
            reach = 1
            while reach < WINDOWS[g]:
                totals = totals + delayed(totals, reach)
                reach = reach * 2
            pooled[:, t * local : (t + 1) * local] = (totals * share - normed).astype(BF16)
        mixed = jnp.dot(pooled[...], pool_full[g], preferred_element_type=F32)
        middle[:, part] = (
            mixed * pool_scale[:, part] + residual[:, part].astype(F32)
        ).astype(BF16)

    middle_copy = local_copy(middle, middle_all.at[tp], 0)
    for d in range(1, n_tp):
        start(
            remote(middle, middle_all.at[tp], tp_send.at[2, d - 1], tp_recv.at[2, d - 1], "tp", d)
        )
    for step in range(1, n_fs - 1):
        for w in (0, 1):
            if step == n_fs - 2 and n_fs > 2:
                break
            for sub in range(SUBS):
                serve(w, sub, step)
    for sub in range(SUBS):
        if n_fs > 1:
            start(ring(2, sub, 0))
    for d in range(1, n_fs):
        got = scales_all.at[other("fs", n_fs - d)]
        remote(got, got, scale_send.at[d - 1], scale_recv.at[d - 1], "fs", d).wait_recv()
    shard_columns = scale_pair.shape[1]
    for f in range(n_fs):
        scale_row[:, f * shard_columns : (f + 1) * shard_columns] = scales_all[f]

    middle_copy.wait()
    tp_arrivals(2, middle_all)
    factor = mean_square_root(middle_all)
    for t in range(n_tp):
        for g in range(groups):
            part = slice(g * local, (g + 1) * local)
            start_column = g * channels + t * local
            inputs[:, start_column : start_column + local] = (
                middle_all[t, :, part].astype(F32) * factor * gains_all[t, 1:2, part]
            ).astype(BF16)

    def finish(w):
        if n_fs > 2:
            for sub in range(SUBS):
                serve(w, sub, n_fs - 2)
        for step in range(n_fs - 1):
            settle(w, step)

    def product(full, columns, row):
        block = full[:, :, columns].reshape(width, COLUMNS)
        made = jnp.dot(inputs[...], block, preferred_element_type=F32)
        return (made * scale_row[row : row + 1, columns]).astype(BF16)

    chunks = gate_full.shape[2] // COLUMNS

    finish(0)

    @pl.loop(0, chunks)
    def _(j):
        columns = pl.ds(pl.multiple_of(j * COLUMNS, COLUMNS), COLUMNS)
        gate_pre[:, columns] = product(gate_full, columns, 0)

    finish(1)
    for sub in range(SUBS):
        if n_fs > 1:
            serve(2, sub, 0)

    @pl.loop(0, chunks)
    def _(j):
        columns = pl.ds(pl.multiple_of(j * COLUMNS, COLUMNS), COLUMNS)
        up_values = product(up_full, columns, 1).astype(F32)
        conv_gate = causal_taps(gate_pre[:, columns].astype(F32), gate_taps[:, columns])
        conv_up = causal_taps(up_values, up_taps[:, columns])
        silu = conv_gate / (1.0 + jnp.exp(-conv_gate))
        hidden[:, columns] = (silu * conv_up).astype(BF16)

    shard_width = down_own.shape[1]

    def to_peers(idx, src, dst):
        for d in range(1, n_tp):
            start(
                remote(
                    src(other("tp", d)),
                    dst(tp),
                    part_send.at[idx, d - 1],
                    part_recv.at[idx, d - 1],
                    "tp",
                    d,
                )
            )

    def from_peers(idx, dst):
        for d in range(1, n_tp):
            got = dst(other("tp", n_tp - d))
            remote(
                got, got, part_send.at[idx, d - 1], part_recv.at[idx, d - 1], "tp", d
            ).wait_recv()

    def conclude(g, columns):
        total = partials[tp, g].astype(F32)
        for d in range(1, n_tp):
            total = total + arrived[other("tp", d), g].astype(F32)
        out[:, columns] = (
            total * down_scale[:, columns] + middle[:, columns].astype(F32)
        ).astype(BF16)

    if shard_width == channels and local % 128 == 0:
        for step in range(n_fs):
            shard = lax.rem(fs - step + n_fs, n_fs)
            if step >= 1:
                if step >= 2:
                    for sub in range(SUBS):
                        serve(2, sub, step - 1)
                settle(2, step - 1)
            made = jnp.dot(hidden[...], down_full[shard], preferred_element_type=F32)
            for t in range(n_tp):
                partials[t, shard] = made[:, t * local : (t + 1) * local].astype(BF16)
            to_peers(step, lambda t: partials.at[t, shard], lambda t: arrived.at[t, shard])
        for step in range(n_fs):
            shard = lax.rem(fs - step + n_fs, n_fs)
            from_peers(step, lambda t: arrived.at[t, shard])
            conclude(shard, pl.ds(pl.multiple_of(shard * local, local), local))
    else:
        for step in range(n_fs - 1):
            if step >= 1:
                for sub in range(SUBS):
                    serve(2, sub, step)
            settle(2, step)
        for f in range(n_fs):
            made = jnp.dot(hidden[...], down_full[f], preferred_element_type=F32).astype(BF16)
            span = min(local, shard_width)
            for at in range(0, shard_width, span):
                g, channel = divmod(f * shard_width + at, channels)
                t, low = divmod(channel, local)
                partials[t, g, :, low : low + span] = made[:, at : at + span]
        to_peers(0, lambda t: partials.at[t], lambda t: arrived.at[t])
        from_peers(0, lambda t: arrived.at[t])
        for g in range(groups):
            conclude(g, slice(g * local, (g + 1) * local))

    for copy in sent:
        copy.wait_send()


def shards(
    sizes,
    residual,
    mixer_gain,
    pool_weight,
    pool_scale,
    channel_gain,
    gate_weight,
    up_weight,
    gate_scale,
    up_scale,
    gate_taps,
    up_taps,
    down_weight,
    down_scale,
):
    n_rep, n_fs, n_tp = sizes
    _, length, groups, local = residual.shape
    channels = local * n_tp
    width = groups * channels
    own_width = groups * local
    hidden_width = gate_weight.shape[1]
    vmem = pl.BlockSpec(memory_space=pltpu.VMEM)
    anywhere = pl.BlockSpec(memory_space=pl.ANY)
    dma = pltpu.SemaphoreType.DMA
    hops = max(n_fs - 1, 1)
    reps = max(n_rep - 1, 1)
    peers = max(n_tp - 1, 1)
    out = pl.pallas_call(
        functools.partial(block_kernel, sizes),
        out_shape=jax.ShapeDtypeStruct((length, own_width), BF16),
        in_specs=[vmem] * 8 + [anywhere] * 3,
        out_specs=vmem,
        scratch_shapes=[
            pltpu.VMEM((groups, channels, local), BF16),
            pltpu.VMEM((n_fs,) + gate_weight.shape, BF16),
            pltpu.VMEM((n_fs,) + up_weight.shape, BF16),
            pltpu.VMEM((n_fs,) + down_weight.shape, BF16),
            pltpu.VMEM((n_tp, length, own_width), BF16),
            pltpu.VMEM((n_tp, length, own_width), BF16),
            pltpu.VMEM((n_tp, 2, own_width), F32),
            pltpu.VMEM((n_fs, 2, gate_scale.shape[1]), F32),
            pltpu.VMEM((2, hidden_width), F32),
            pltpu.VMEM((length, channels), BF16),
            pltpu.VMEM((length, own_width), BF16),
            pltpu.VMEM((length, width), BF16),
            pltpu.VMEM((length, hidden_width), BF16),
            pltpu.VMEM((length, hidden_width), BF16),
            pltpu.VMEM((n_tp, groups, length, local), BF16),
            pltpu.VMEM((n_tp, groups, length, local), BF16),
            dma((3, SUBS, hops)),
            dma((3, SUBS, hops)),
            dma((3, SUBS, hops, reps)),
            dma((3, SUBS, hops, reps)),
            dma((hops,)),
            dma((hops,)),
            dma((hops, reps)),
            dma((hops, reps)),
            dma((hops,)),
            dma((hops,)),
            dma((3, peers)),
            dma((3, peers)),
            dma((n_fs, peers)),
            dma((n_fs, peers)),
            dma((7,)),
        ],
        compiler_params=pltpu.CompilerParams(
            collective_id=0, has_side_effects=True, vmem_limit_bytes=60 * 1024 * 1024
        ),
    )(
        residual.reshape(length, own_width),
        jnp.stack([mixer_gain.reshape(-1), channel_gain.reshape(-1)]),
        pool_scale.reshape(1, -1),
        down_scale.reshape(1, -1),
        jnp.concatenate([gate_scale, up_scale], axis=0),
        gate_taps,
        up_taps,
        pool_weight.astype(BF16),
        gate_weight.astype(BF16),
        up_weight.astype(BF16),
        down_weight.astype(BF16),
    )
    return out.reshape(1, length, groups, local)


def solution(mesh):
    placed = (
        P(("rep", "fs"), None, None, "tp"),
        P(None, "tp"),
        P(None, "fs", "tp"),
        P(None, "tp"),
        P(None, "tp"),
        P("fs", "tp"),
        P("fs", "tp"),
        P("fs", "tp"),
        P("fs", "tp"),
        P(None, "tp"),
        P(None, "tp"),
        P("tp", "fs"),
        P(None, "tp"),
    )
    sizes = tuple(mesh.shape[name] for name in ("rep", "fs", "tp"))
    return jax.shard_map(
        functools.partial(shards, sizes),
        mesh=mesh,
        in_specs=placed,
        out_specs=P(("rep", "fs"), None, None, "tp"),
        check_vma=False,
    )
```

```python
import functools

import jax
import jax.numpy as jnp
from jax import lax
from jax.experimental import pallas as pl
from jax.experimental.pallas import tpu as pltpu
from jax.sharding import PartitionSpec as P

WINDOWS = (2, 4, 8, 16)
EPSILON = 1e-05
SUBS = 2
COLUMNS = 256
F32 = jnp.float32
BF16 = jnp.bfloat16


def delayed(values, steps):
    rows = lax.broadcasted_iota(jnp.int32, values.shape, 0)
    return jnp.where(rows >= steps, pltpu.roll(values, steps, 0), 0.0)


def causal_taps(values, taps):
    return taps[2:3] * values + taps[1:2] * delayed(values, 1) + taps[0:1] * delayed(values, 2)


def block_kernel(
    sizes,
    residual,
    gains,
    pool_scale,
    down_scale,
    scale_pair,
    gate_taps,
    up_taps,
    pool_own,
    gate_own,
    up_own,
    down_own,
    out,
    pool_full,
    gate_full,
    up_full,
    down_full,
    gathered,
    middle_all,
    gains_all,
    scales_all,
    scale_row,
    pooled,
    middle,
    inputs,
    gate_pre,
    hidden,
    partials,
    arrived,
    ring_send,
    ring_recv,
    rep_send,
    rep_recv,
    pool_send,
    pool_recv,
    pool_rep_send,
    pool_rep_recv,
    scale_send,
    scale_recv,
    tp_send,
    tp_recv,
    part_send,
    part_recv,
    local_sem,
):
    n_rep, n_fs, n_tp = sizes
    rep, fs, tp = (lax.axis_index(name) for name in ("rep", "fs", "tp"))
    length = residual.shape[0]
    groups = pool_full.shape[0]
    channels = pool_full.shape[1]
    local = residual.shape[1] // groups
    width = groups * channels

    def other(axis, offset):
        me, count = {"rep": (rep, n_rep), "fs": (fs, n_fs), "tp": (tp, n_tp)}[axis]
        return lax.rem(me + offset, count)

    def remote(src, dst, send, recv, axis, offset):
        return pltpu.make_async_remote_copy(
            src_ref=src,
            dst_ref=dst,
            send_sem=send,
            recv_sem=recv,
            device_id={axis: other(axis, offset)},
            device_id_type=pl.DeviceIdType.MESH,
        )

    barrier = pltpu.get_barrier_semaphore()
    for axis, count in (("rep", n_rep), ("fs", n_fs), ("tp", n_tp)):
        for offset in range(1, count):
            pl.semaphore_signal(
                barrier,
                inc=1,
                device_id={axis: other(axis, offset)},
                device_id_type=pl.DeviceIdType.MESH,
            )
    pl.semaphore_wait(barrier, n_rep + n_fs + n_tp - 3)

    sent = []

    def start(copy, valid=None):
        sent.append((copy, valid))
        if valid is None:
            copy.start()
        else:
            pl.when(valid)(copy.start)

    weights = ((gate_own, gate_full), (up_own, up_full), (down_own, down_full))

    def piece(w, shard, half, sub, own=False):
        rows = weights[w][0].shape[0] // (n_rep * SUBS)
        part = pl.ds(pl.multiple_of((half * SUBS + sub) * rows, rows), rows)
        return weights[w][0].at[part] if own else weights[w][1].at[shard, part]

    def shard_sent(step, way):
        shard = fs + step if way else fs - step
        return jnp.clip(shard, 0, n_fs - 1), (shard <= n_fs - 1 if way else shard >= 0)

    def line(w, sub, step):
        for way in range(2):
            shard, valid = shard_sent(step, way)
            start(
                remote(
                    piece(w, shard, rep, sub, own=step == 0),
                    piece(w, shard, rep, sub),
                    ring_send.at[w, sub, 2 * step + way],
                    ring_recv.at[w, sub, 2 * step + way],
                    "fs",
                    n_fs - 1 if way else 1,
                ),
                valid & (fs > 0 if way else fs < n_fs - 1),
            )

    def serve(w, sub, step):
        for way in range(2):
            shard, valid = shard_sent(step + 1, way)
            mine = piece(w, shard, rep, sub)
            sems = (w, sub, 2 * step + way)
            pl.when(valid)(
                remote(
                    mine, mine, ring_send.at[sems], ring_recv.at[sems], "fs", 1
                ).wait_recv
            )
            if step < n_fs - 2:
                onward = (w, sub, 2 * step + 2 + way)
                start(
                    remote(
                        mine,
                        mine,
                        ring_send.at[onward],
                        ring_recv.at[onward],
                        "fs",
                        n_fs - 1 if way else 1,
                    ),
                    valid & (fs > 0 if way else fs < n_fs - 1),
                )
            for d in range(1, n_rep):
                start(
                    remote(
                        mine,
                        mine,
                        rep_send.at[sems + (d - 1,)],
                        rep_recv.at[sems + (d - 1,)],
                        "rep",
                        d,
                    ),
                    valid,
                )

    def settle(w, step, ways=(0, 1)):
        for way in ways:
            shard, valid = shard_sent(step + 1, way)

            @pl.when(valid)
            def _():
                for sub in range(SUBS):
                    for d in range(1, n_rep):
                        got = piece(w, shard, other("rep", n_rep - d), sub)
                        sems = (w, sub, 2 * step + way, d - 1)
                        remote(
                            got, got, rep_send.at[sems], rep_recv.at[sems], "rep", d
                        ).wait_recv()

    def local_copy(src, dst, idx):
        copy = pltpu.make_async_copy(src, dst, local_sem.at[idx])
        copy.start()
        return copy

    own_copies = [
        local_copy(residual, gathered.at[tp], 0),
        local_copy(gains, gains_all.at[tp], 1),
        local_copy(scale_pair, scales_all.at[fs], 2),
        local_copy(gate_own, gate_full.at[fs], 3),
        local_copy(up_own, up_full.at[fs], 4),
        local_copy(down_own, down_full.at[fs], 5),
    ]

    pool_rows = pool_own.shape[1]
    rep_groups = groups // n_rep

    def pool_part(shard, half):
        return pool_full.at[
            pl.ds(half * rep_groups, rep_groups),
            pl.ds(pl.multiple_of(shard * pool_rows, pool_rows), pool_rows),
        ]

    pool_copy = local_copy(
        pool_own, pool_full.at[:, pl.ds(pl.multiple_of(fs * pool_rows, pool_rows), pool_rows)], 6
    )

    for d in range(1, n_fs):
        start(
            remote(
                pool_own.at[pl.ds(rep * rep_groups, rep_groups)],
                pool_part(fs, rep),
                pool_send.at[d - 1],
                pool_recv.at[d - 1],
                "fs",
                d,
            )
        )
    for w in (0, 1):
        for sub in range(SUBS):
            if n_fs > 1:
                line(w, sub, 0)
    for d in range(1, n_tp):
        start(remote(gains, gains_all.at[tp], tp_send.at[0, d - 1], tp_recv.at[0, d - 1], "tp", d))
    for d in range(1, n_tp):
        start(
            remote(residual, gathered.at[tp], tp_send.at[1, d - 1], tp_recv.at[1, d - 1], "tp", d)
        )
    for d in range(1, n_fs):
        start(
            remote(
                scale_pair, scales_all.at[fs], scale_send.at[d - 1], scale_recv.at[d - 1], "fs", d
            )
        )

    for d in range(1, n_fs):
        shard = other("fs", n_fs - d)
        mine = pool_part(shard, rep)
        remote(mine, mine, pool_send.at[d - 1], pool_recv.at[d - 1], "fs", d).wait_recv()
        for e in range(1, n_rep):
            start(
                remote(
                    mine,
                    mine,
                    pool_rep_send.at[d - 1, e - 1],
                    pool_rep_recv.at[d - 1, e - 1],
                    "rep",
                    e,
                )
            )
    for d in range(1, n_fs):
        shard = other("fs", n_fs - d)
        for e in range(1, n_rep):
            got = pool_part(shard, other("rep", n_rep - e))
            remote(
                got,
                got,
                pool_rep_send.at[d - 1, e - 1],
                pool_rep_recv.at[d - 1, e - 1],
                "rep",
                e,
            ).wait_recv()
    pool_copy.wait()
    for copy in own_copies:
        copy.wait()

    def tp_arrivals(idx, buffer):
        for d in range(1, n_tp):
            got = buffer.at[other("tp", n_tp - d)]
            remote(got, got, tp_send.at[idx, d - 1], tp_recv.at[idx, d - 1], "tp", d).wait_recv()

    for sub in range(SUBS):
        serve(0, sub, 0)
    tp_arrivals(0, gains_all)
    tp_arrivals(1, gathered)
    for sub in range(SUBS):
        serve(1, sub, 0)

    def mean_square_root(buffer):
        total = jnp.zeros((length, 1), F32)
        for t in range(n_tp):
            values = buffer[t].astype(F32)
            total = total + jnp.sum(values * values, axis=1, keepdims=True)
        return lax.rsqrt(total / width + EPSILON)

    factor = mean_square_root(gathered)
    positions = lax.broadcasted_iota(jnp.int32, (length, 1), 0).astype(F32) + 1.0
    for g in range(groups):
        part = slice(g * local, (g + 1) * local)
        share = 1.0 / jnp.minimum(positions, float(WINDOWS[g]))
        for t in range(n_tp):
            values = gathered[t, :, part].astype(F32)
            normed = (values * factor * gains_all[t, 0:1, part]).astype(BF16).astype(F32)
            totals = normed
            reach = 1
            while reach < WINDOWS[g]:
                totals = totals + delayed(totals, reach)
                reach = reach * 2
            pooled[:, t * local : (t + 1) * local] = (totals * share - normed).astype(BF16)
        mixed = jnp.dot(pooled[...], pool_full[g], preferred_element_type=F32)
        middle[:, part] = (
            mixed * pool_scale[:, part] + residual[:, part].astype(F32)
        ).astype(BF16)

    middle_copy = local_copy(middle, middle_all.at[tp], 0)
    for d in range(1, n_tp):
        start(
            remote(middle, middle_all.at[tp], tp_send.at[2, d - 1], tp_recv.at[2, d - 1], "tp", d)
        )
    for step in range(1, n_fs - 1):
        for w in (0, 1):
            if step == n_fs - 2 and n_fs > 2:
                break
            for sub in range(SUBS):
                serve(w, sub, step)
    for sub in range(SUBS):
        if n_fs > 1:
            line(2, sub, 0)
    for d in range(1, n_fs):
        got = scales_all.at[other("fs", n_fs - d)]
        remote(got, got, scale_send.at[d - 1], scale_recv.at[d - 1], "fs", d).wait_recv()
    shard_columns = scale_pair.shape[1]
    for f in range(n_fs):
        scale_row[:, f * shard_columns : (f + 1) * shard_columns] = scales_all[f]

    middle_copy.wait()
    tp_arrivals(2, middle_all)
    factor = mean_square_root(middle_all)
    for t in range(n_tp):
        for g in range(groups):
            part = slice(g * local, (g + 1) * local)
            start_column = g * channels + t * local
            inputs[:, start_column : start_column + local] = (
                middle_all[t, :, part].astype(F32) * factor * gains_all[t, 1:2, part]
            ).astype(BF16)

    def finish(w):
        if n_fs > 2:
            for sub in range(SUBS):
                serve(w, sub, n_fs - 2)
        for step in range(n_fs - 1):
            settle(w, step)

    def product(full, columns, row):
        block = full[:, :, columns].reshape(width, COLUMNS)
        made = jnp.dot(inputs[...], block, preferred_element_type=F32)
        return (made * scale_row[row : row + 1, columns]).astype(BF16)

    chunks = gate_full.shape[2] // COLUMNS

    finish(0)

    @pl.loop(0, chunks)
    def _(j):
        columns = pl.ds(pl.multiple_of(j * COLUMNS, COLUMNS), COLUMNS)
        gate_pre[:, columns] = product(gate_full, columns, 0)

    finish(1)
    for sub in range(SUBS):
        if n_fs > 1:
            serve(2, sub, 0)

    @pl.loop(0, chunks)
    def _(j):
        columns = pl.ds(pl.multiple_of(j * COLUMNS, COLUMNS), COLUMNS)
        up_values = product(up_full, columns, 1).astype(F32)
        conv_gate = causal_taps(gate_pre[:, columns].astype(F32), gate_taps[:, columns])
        conv_up = causal_taps(up_values, up_taps[:, columns])
        silu = conv_gate / (1.0 + jnp.exp(-conv_gate))
        hidden[:, columns] = (silu * conv_up).astype(BF16)

    shard_width = down_own.shape[1]

    def to_peers(idx, src, dst):
        for d in range(1, n_tp):
            start(
                remote(
                    src(other("tp", d)),
                    dst(tp),
                    part_send.at[idx, d - 1],
                    part_recv.at[idx, d - 1],
                    "tp",
                    d,
                )
            )

    def from_peers(idx, dst):
        for d in range(1, n_tp):
            got = dst(other("tp", n_tp - d))
            remote(
                got, got, part_send.at[idx, d - 1], part_recv.at[idx, d - 1], "tp", d
            ).wait_recv()

    def conclude(g, columns):
        total = partials[tp, g].astype(F32)
        for d in range(1, n_tp):
            total = total + arrived[other("tp", d), g].astype(F32)
        out[:, columns] = (
            total * down_scale[:, columns] + middle[:, columns].astype(F32)
        ).astype(BF16)

    if shard_width == channels and local % 128 == 0:
        def share(shard):
            made = jnp.dot(hidden[...], down_full[shard], preferred_element_type=F32)
            for t in range(n_tp):
                partials[t, shard] = made[:, t * local : (t + 1) * local].astype(BF16)
            for d in range(1, n_tp):
                peer = other("tp", d)
                remote(
                    partials.at[peer, shard],
                    arrived.at[tp, shard],
                    part_send.at[shard, d - 1],
                    part_recv.at[shard, d - 1],
                    "tp",
                    d,
                ).start()

        share(fs)
        for step in range(n_fs - 1):
            if step >= 1:
                for sub in range(SUBS):
                    serve(2, sub, step)
            for way in range(2):
                settle(2, step, (way,))
                shard, valid = shard_sent(step + 1, way)
                pl.when(valid)(functools.partial(share, shard))
        for shard in range(n_fs):
            from_peers(shard, lambda t: arrived.at[t, shard])
            conclude(shard, slice(shard * local, (shard + 1) * local))
            for d in range(1, n_tp):
                mine = partials.at[other("tp", d), shard]
                remote(
                    mine, mine, part_send.at[shard, d - 1], part_recv.at[shard, d - 1], "tp", d
                ).wait_send()
    else:
        for step in range(n_fs - 1):
            if step >= 1:
                for sub in range(SUBS):
                    serve(2, sub, step)
            settle(2, step)
        for f in range(n_fs):
            made = jnp.dot(hidden[...], down_full[f], preferred_element_type=F32).astype(BF16)
            span = min(local, shard_width)
            for at in range(0, shard_width, span):
                g, channel = divmod(f * shard_width + at, channels)
                t, low = divmod(channel, local)
                partials[t, g, :, low : low + span] = made[:, at : at + span]
        to_peers(0, lambda t: partials.at[t], lambda t: arrived.at[t])
        from_peers(0, lambda t: arrived.at[t])
        for g in range(groups):
            conclude(g, slice(g * local, (g + 1) * local))

    for copy, valid in sent:
        if valid is None:
            copy.wait_send()
        else:
            pl.when(valid)(copy.wait_send)


def shards(
    sizes,
    residual,
    mixer_gain,
    pool_weight,
    pool_scale,
    channel_gain,
    gate_weight,
    up_weight,
    gate_scale,
    up_scale,
    gate_taps,
    up_taps,
    down_weight,
    down_scale,
):
    n_rep, n_fs, n_tp = sizes
    _, length, groups, local = residual.shape
    channels = local * n_tp
    width = groups * channels
    own_width = groups * local
    hidden_width = gate_weight.shape[1]
    vmem = pl.BlockSpec(memory_space=pltpu.VMEM)
    anywhere = pl.BlockSpec(memory_space=pl.ANY)
    dma = pltpu.SemaphoreType.DMA
    hops = max(n_fs - 1, 1)
    reps = max(n_rep - 1, 1)
    peers = max(n_tp - 1, 1)
    out = pl.pallas_call(
        functools.partial(block_kernel, sizes),
        out_shape=jax.ShapeDtypeStruct((length, own_width), BF16),
        in_specs=[vmem] * 8 + [anywhere] * 3,
        out_specs=vmem,
        scratch_shapes=[
            pltpu.VMEM((groups, channels, local), BF16),
            pltpu.VMEM((n_fs,) + gate_weight.shape, BF16),
            pltpu.VMEM((n_fs,) + up_weight.shape, BF16),
            pltpu.VMEM((n_fs,) + down_weight.shape, BF16),
            pltpu.VMEM((n_tp, length, own_width), BF16),
            pltpu.VMEM((n_tp, length, own_width), BF16),
            pltpu.VMEM((n_tp, 2, own_width), F32),
            pltpu.VMEM((n_fs, 2, gate_scale.shape[1]), F32),
            pltpu.VMEM((2, hidden_width), F32),
            pltpu.VMEM((length, channels), BF16),
            pltpu.VMEM((length, own_width), BF16),
            pltpu.VMEM((length, width), BF16),
            pltpu.VMEM((length, hidden_width), BF16),
            pltpu.VMEM((length, hidden_width), BF16),
            pltpu.VMEM((n_tp, groups, length, local), BF16),
            pltpu.VMEM((n_tp, groups, length, local), BF16),
            dma((3, SUBS, 2 * hops)),
            dma((3, SUBS, 2 * hops)),
            dma((3, SUBS, 2 * hops, reps)),
            dma((3, SUBS, 2 * hops, reps)),
            dma((hops,)),
            dma((hops,)),
            dma((hops, reps)),
            dma((hops, reps)),
            dma((hops,)),
            dma((hops,)),
            dma((3, peers)),
            dma((3, peers)),
            dma((n_fs, peers)),
            dma((n_fs, peers)),
            dma((7,)),
        ],
        compiler_params=pltpu.CompilerParams(
            collective_id=0, has_side_effects=True, vmem_limit_bytes=60 * 1024 * 1024
        ),
    )(
        residual.reshape(length, own_width),
        jnp.stack([mixer_gain.reshape(-1), channel_gain.reshape(-1)]),
        pool_scale.reshape(1, -1),
        down_scale.reshape(1, -1),
        jnp.concatenate([gate_scale, up_scale], axis=0),
        gate_taps,
        up_taps,
        pool_weight.astype(BF16),
        gate_weight.astype(BF16),
        up_weight.astype(BF16),
        down_weight.astype(BF16),
    )
    return out.reshape(1, length, groups, local)


def solution(mesh):
    placed = (
        P(("rep", "fs"), None, None, "tp"),
        P(None, "tp"),
        P(None, "fs", "tp"),
        P(None, "tp"),
        P(None, "tp"),
        P("fs", "tp"),
        P("fs", "tp"),
        P("fs", "tp"),
        P("fs", "tp"),
        P(None, "tp"),
        P(None, "tp"),
        P("tp", "fs"),
        P(None, "tp"),
    )
    sizes = tuple(mesh.shape[name] for name in ("rep", "fs", "tp"))
    return jax.shard_map(
        functools.partial(shards, sizes),
        mesh=mesh,
        in_specs=placed,
        out_specs=P(("rep", "fs"), None, None, "tp"),
        check_vma=False,
    )
```
